32 devices in a mesh: ep: 8 (over z, core), tp: 4 (over y, x).
Axes of the slice: x: 2, y: 2, z: 4, core: 2. Of those that a mesh axis runs over, the one named last changes fastest.
Arguments:
- tokens: bfloat16 [1024, 2048], P('ep'), may hold values from -6 to 6
- chosen: int32 [8, 8, 8], replicated, may hold values from 0 to 127, as said below
- chosen_weight: float32 [8, 8, 8], P('ep'), may hold values from 0.1 to 1
- gate_weight: bfloat16 [8, 2048, 4096], P('ep', None, 'tp'), may hold values from -0.125 to 0.125
- up_weight: bfloat16 [8, 2048, 4096], P('ep', None, 'tp'), may hold values from -0.125 to 0.125
- down_weight: bfloat16 [8, 4096, 2048], P('ep', 'tp'), may hold values from -0.09375 to 0.09375
Outputs:
- combined: bfloat16 [1024, 2048], P('ep', 'tp')
The draws below stay inside these ranges and needn't reach their ends.
Inputs may be any that keep to these rules, and one draw needn't show every extreme that they name: `chosen`: for every block and expert the 8 positions are distinct.
All inputs are finite; a program needn't handle non-finite values.
Results may differ from the reference program's by a relative error of at most 0.015.
Values may be sent and summed in bfloat16 or wider, within the bound.
A program may use at most 64 MiB of HBM per device.

```python
import jax
import jax.numpy as jnp
from jax import lax

D = 2048
FF = 4096
TOK_DEV = 128
PICK = 8
BLOCKS = 8
EXPERTS = 8
TOKENS = 1024
N_TP = 4


def draw_chosen(key, part):
    keys = jax.random.split(jax.random.fold_in(key, 11), BLOCKS * EXPERTS)
    orders = jax.vmap(lambda single: jax.random.permutation(single, TOK_DEV)[:PICK])(keys)
    return orders.reshape(BLOCKS, EXPERTS, PICK).astype(jnp.int32)


def shard_levels(stream_key, dims, cuts, low, top_value):
    def one(dim, blocks):
        draws = jax.random.uniform(jax.random.fold_in(jax.random.fold_in(stream_key, 6), dim), (blocks,), jnp.float32, low / len(cuts), top_value / len(cuts))
        return jnp.repeat(jnp.exp(draws), dims[dim] // blocks).reshape((-1,) + (1,) * (len(dims) - dim - 1))

    gain = one(*cuts[0])
    for cut in cuts[1:]:
        gain = gain * one(*cut)
    return gain


def gaussian(own_key, extent, width, most, cuts=(), kind=jnp.bfloat16):
    loudness = shard_levels(own_key, extent, cuts, -0.22, 0.18) if cuts else 1.0
    values = jax.random.normal(own_key, extent, jnp.float32) * width * loudness
    return jnp.minimum(jnp.maximum(values, -most), most).astype(kind)


def setup_inputs(seed: int = 0) -> dict:
    splits = jax.random.split(jax.random.key(seed), 7)
    tokens = gaussian(splits[0], (TOKENS, D), 1.0, 6.0, ((0, 8),))
    chosen = draw_chosen(jax.random.fold_in(splits[6], 71), 0)
    chosen_weight = jnp.clip(0.1 + 0.9 * jax.random.uniform(splits[2], (BLOCKS, EXPERTS, PICK), jnp.float32) ** shard_levels(splits[2], (BLOCKS, EXPERTS, PICK), ((0, 8),), -0.2, 0.2), 0.1, 1.0)
    gate_weight = gaussian(splits[3], (EXPERTS, D, FF), D ** -0.5, 0.125, ((0, 8), (2, 4)))
    up_weight = gaussian(splits[4], (EXPERTS, D, FF), D ** -0.5, 0.125, ((0, 8), (2, 4)))
    down_weight = gaussian(splits[5], (EXPERTS, FF, D), FF ** -0.5, 0.09375, ((0, 8), (1, 4)))
    return {"tokens": tokens, "chosen": chosen, "chosen_weight": chosen_weight, "gate_weight": gate_weight, "up_weight": up_weight, "down_weight": down_weight}


def reference(tokens, chosen, chosen_weight, gate_weight, up_weight, down_weight):
    offsets = (jnp.arange(BLOCKS, dtype=jnp.int32) * TOK_DEV)[:, None, None]
    global_rows = (chosen + offsets).astype(jnp.int32)
    per_expert = jnp.transpose(global_rows, (1, 0, 2)).reshape(EXPERTS, BLOCKS * PICK)
    slice_width = FF // N_TP

    def expert_pass(inputs):
        picked, gate_local, up_local, down_local = inputs
        selected = jnp.take(tokens, picked, axis=0)
        gate_sum = jnp.dot(selected, gate_local, preferred_element_type=jnp.float32)
        up_sum = jnp.dot(selected, up_local, preferred_element_type=jnp.float32)
        hidden = (jax.nn.silu(gate_sum) * up_sum).astype(jnp.bfloat16)
        partials = jnp.einsum("rtf,tfd->trd",
                              hidden.reshape(-1, N_TP, slice_width).astype(jnp.float32),
                              down_local.reshape(N_TP, slice_width, D).astype(jnp.float32))
        rounded = lax.optimization_barrier(partials.astype(jnp.bfloat16))
        return jnp.sum(rounded.astype(jnp.float32), axis=0).astype(jnp.bfloat16)

    outputs = lax.map(expert_pass, (per_expert, gate_weight, up_weight, down_weight))
    arranged = jnp.transpose(outputs.reshape(EXPERTS, BLOCKS, PICK, D), (1, 0, 2, 3))
    weighted = arranged.astype(jnp.float32) * chosen_weight[..., None]
    combined = jnp.zeros((BLOCKS * TOK_DEV, D), jnp.float32).at[global_rows.reshape(-1)].add(weighted.reshape(-1, D))
    return combined.astype(jnp.bfloat16)
```

```python
import functools

import jax
import jax.numpy as jnp
from jax import lax
from jax.experimental import pallas as pl
from jax.experimental.pallas import tpu as pltpu
from jax.sharding import PartitionSpec as P

MESH = pl.DeviceIdType.MESH
CHUNKS = 4


def each(count, body):
    if count <= 8:
        for i in range(count):
            body(i)
    else:
        pl.loop(0, count)(body)


def partner(t, j, count):
    if count & (count - 1):
        return lax.rem(t + j, count)
    out, bit = 0, 1
    while bit < count:
        have = (t // bit) % 2
        out = out + ((have + 1) % 2 if j & bit else have) * bit
        bit *= 2
    return out


def kernel(
    n_ep, n_tp,
    tok_hbm, cho_hbm, wt_hbm, gate_hbm, up_hbm, down_hbm,
    out_ref,
    tok, cho, wt, gate, up, down,
    leaving, arrived, gate_acc, up_acc, place,
    part_out, part_in, back_out, back_in,
    in_sem, w_sem, d_sem,
    s1_send, s1_recv, s2_send, s2_recv, s3_send, s3_recv,
):
    e = lax.axis_index("ep")
    t = lax.axis_index("tp")
    tok_count, width = tok.shape
    experts, picks = cho.shape
    rows = experts * picks
    cw = width // CHUNKS
    sw = width // n_tp
    hid = gate.shape[1]

    def ep_peer(j):
        low = n_ep - 1 - j
        low = jnp.where(low > e, low, low - 1)
        high = jnp.where(j < e, j, j + 1)
        return jnp.where(e < n_ep // 2, low, high)

    barrier = pltpu.get_barrier_semaphore()

    def greet(j):
        pl.semaphore_signal(barrier, inc=1, device_id={"ep": ep_peer(j)}, device_id_type=MESH)

    each(n_ep - 1, greet)
    for j in range(1, n_tp):
        pl.semaphore_signal(
            barrier, inc=1, device_id={"tp": partner(t, j, n_tp)}, device_id_type=MESH
        )

    loads = [
        pltpu.make_async_copy(cho_hbm.at[e], cho, in_sem.at[0]),
        pltpu.make_async_copy(wt_hbm.at[0], wt, in_sem.at[1]),
        pltpu.make_async_copy(tok_hbm, tok, in_sem.at[2]),
    ]
    for c in loads:
        c.start()
    wloads = []
    for k in range(CHUNKS):
        piece = pl.ds(k * cw, cw)
        a = pltpu.make_async_copy(gate_hbm.at[0, piece, :], gate.at[piece, :], w_sem.at[0, k])
        b = pltpu.make_async_copy(up_hbm.at[0, piece, :], up.at[piece, :], w_sem.at[1, k])
        a.start()
        b.start()
        wloads.append((a, b))
    order = [*range(n_tp - 1, 0, -1), 0]
    dloads = {}
    for j in order:
        col = pl.multiple_of(partner(t, j, n_tp) * sw, sw)
        dloads[j] = pltpu.make_async_copy(
            down_hbm.at[0, :, pl.ds(col, sw)], down.at[j], d_sem.at[j]
        )
        dloads[j].start()

    for c in loads:
        c.wait()
    lane = lax.broadcasted_iota(jnp.int32, (picks, picks), 1)
    sub = lax.broadcasted_iota(jnp.int32, (picks, picks), 0)
    diag = lane == sub
    position = lax.broadcasted_iota(jnp.int32, (picks, tok_count), 1).astype(jnp.float32)
    hots, parts = [], []
    for x in range(experts):
        spread = jnp.broadcast_to(cho[x : x + 1, :], (picks, picks)).astype(jnp.float32)
        column = jnp.sum(jnp.where(diag, spread, 0.0), axis=1, keepdims=True)
        wide = jnp.broadcast_to(wt[x : x + 1, :], (picks, picks))
        wcol = jnp.sum(jnp.where(diag, wide, 0.0), axis=1, keepdims=True)
        hit = position == column
        hots.append(jnp.where(hit, 1.0, 0.0))
        parts.append(jnp.where(hit, wcol, 0.0))
    onehot = jnp.concatenate(hots, axis=0).astype(jnp.bfloat16)
    for k in range(CHUNKS):
        sel = jnp.dot(
            onehot, tok[:, k * cw : (k + 1) * cw], preferred_element_type=jnp.float32
        )
        leaving[k] = sel.reshape(experts, picks, cw).astype(jnp.bfloat16)

    pl.semaphore_wait(barrier, n_ep - 1 + n_tp - 1)

    def send_tokens(k, j):
        p = ep_peer(j)
        return pltpu.make_async_remote_copy(
            src_ref=leaving.at[k, p],
            dst_ref=arrived.at[k, e],
            send_sem=s1_send.at[k, j],
            recv_sem=s1_recv.at[k, e],
            device_id={"ep": p},
            device_id_type=MESH,
        )

    for k in range(CHUNKS):
        each(n_ep - 1, lambda j: send_tokens(k, j).start())

    weighted = jnp.concatenate(parts, axis=0)
    hi = weighted.astype(jnp.bfloat16).astype(jnp.float32)
    mid = (weighted - hi).astype(jnp.bfloat16).astype(jnp.float32)
    lo = weighted - hi - mid
    for i, piece in enumerate((hi, mid, lo)):
        place[i] = piece.T.astype(jnp.bfloat16)

    def rows_in(ref, k, sem, p):
        pltpu.make_async_remote_copy(
            src_ref=ref.at[k, p] if k is not None else ref.at[p],
            dst_ref=ref.at[k, p] if k is not None else ref.at[p],
            send_sem=sem.at[k, p] if k is not None else sem.at[p],
            recv_sem=sem.at[k, p] if k is not None else sem.at[p],
            device_id={"ep": p},
            device_id_type=MESH,
        ).wait_recv()

    for k in range(CHUNKS):
        arrived[k, e] = leaving[k, e]
        each(n_ep - 1, lambda j: rows_in(arrived, k, s1_recv, ep_peer(j)))
        x = arrived[k].astype(jnp.float32).reshape(rows, cw).astype(jnp.bfloat16)
        for c in wloads[k]:
            c.wait()
        g = jnp.dot(x, gate[k * cw : (k + 1) * cw, :], preferred_element_type=jnp.float32)
        u = jnp.dot(x, up[k * cw : (k + 1) * cw, :], preferred_element_type=jnp.float32)
        if k == 0:
            gate_acc[...] = g
            up_acc[...] = u
        else:
            gate_acc[...] += g
            up_acc[...] += u
    g = gate_acc[...]
    hidden = (g / (1.0 + jnp.exp(-g)) * up_acc[...]).astype(jnp.bfloat16)

    sends = []
    for j in order:
        dloads[j].wait()
        part_out[j] = jnp.dot(hidden, down[j], preferred_element_type=jnp.float32).astype(
            jnp.bfloat16
        )
        if j:
            c = pltpu.make_async_remote_copy(
                src_ref=part_out.at[j],
                dst_ref=part_in.at[j - 1],
                send_sem=s2_send.at[j - 1],
                recv_sem=s2_recv.at[j - 1],
                device_id={"tp": partner(t, j, n_tp)},
                device_id_type=MESH,
            )
            c.start()
            sends.append(c)
    total = part_out[0].astype(jnp.float32)
    for c in sends:
        c.wait_recv()
    for j in range(1, n_tp):
        total += part_in[j - 1].astype(jnp.float32)
    back_out[...] = total.reshape(n_ep, picks, sw).astype(jnp.bfloat16)

    def send_back(j):
        p = ep_peer(j)
        return pltpu.make_async_remote_copy(
            src_ref=back_out.at[p],
            dst_ref=back_in.at[e],
            send_sem=s3_send.at[j],
            recv_sem=s3_recv.at[e],
            device_id={"ep": p},
            device_id_type=MESH,
        )

    each(n_ep - 1, lambda j: send_back(j).start())
    back_in[e] = back_out[e]
    each(n_ep - 1, lambda j: rows_in(back_in, None, s3_recv, ep_peer(j)))
    y = back_in[...].astype(jnp.float32).reshape(rows, sw).astype(jnp.bfloat16)
    result = jnp.dot(place[0], y, preferred_element_type=jnp.float32)
    result += jnp.dot(place[1], y, preferred_element_type=jnp.float32)
    result += jnp.dot(place[2], y, preferred_element_type=jnp.float32)
    out_ref[...] = result.astype(out_ref.dtype)

    for k in range(CHUNKS):
        each(n_ep - 1, lambda j: send_tokens(k, j).wait_send())
    for c in sends:
        c.wait_send()
    each(n_ep - 1, lambda j: send_back(j).wait_send())


def local(tokens, chosen, chosen_weight, gate_weight, up_weight, down_weight):
    n_ep, n_tp = lax.axis_size("ep"), lax.axis_size("tp")
    tok_count, width = tokens.shape
    blocks, experts, picks = chosen.shape
    hid = gate_weight.shape[2]
    rows = blocks * picks
    cw, sw = width // CHUNKS, width // n_tp
    bf, f32 = jnp.bfloat16, jnp.float32
    dma = pltpu.SemaphoreType.DMA
    hbm = pl.BlockSpec(memory_space=pl.ANY)
    return pl.pallas_call(
        functools.partial(kernel, n_ep, n_tp),
        out_shape=jax.ShapeDtypeStruct((tok_count, sw), bf),
        in_specs=[hbm] * 6,
        out_specs=pl.BlockSpec(memory_space=pltpu.VMEM),
        scratch_shapes=[
            pltpu.VMEM((tok_count, width), bf),
            pltpu.VMEM((experts, picks), jnp.int32),
            pltpu.VMEM((experts, picks), f32),
            pltpu.VMEM((width, hid), bf),
            pltpu.VMEM((width, hid), bf),
            pltpu.VMEM((n_tp, hid, sw), bf),
            pltpu.VMEM((CHUNKS, experts, picks, cw), bf),
            pltpu.VMEM((CHUNKS, blocks, picks, cw), bf),
            pltpu.VMEM((rows, hid), f32),
            pltpu.VMEM((rows, hid), f32),
            pltpu.VMEM((3, tok_count, experts * picks), bf),
            pltpu.VMEM((n_tp, rows, sw), bf),
            pltpu.VMEM((n_tp - 1, rows, sw), bf),
            pltpu.VMEM((blocks, picks, sw), bf),
            pltpu.VMEM((experts, picks, sw), bf),
            dma((3,)),
            dma((2, CHUNKS)),
            dma((n_tp,)),
            dma((CHUNKS, n_ep)),
            dma((CHUNKS, n_ep)),
            dma((n_tp,)),
            dma((n_tp,)),
            dma((n_ep,)),
            dma((n_ep,)),
        ],
        compiler_params=pltpu.CompilerParams(
            collective_id=0, has_side_effects=True, vmem_limit_bytes=60 * 1024 * 1024
        ),
    )(tokens, chosen, chosen_weight, gate_weight, up_weight, down_weight)


def solution(mesh):
    return jax.shard_map(
        local,
        mesh=mesh,
        in_specs=(
            P("ep", None),
            P(),
            P("ep", None, None),
            P("ep", None, "tp"),
            P("ep", None, "tp"),
            P("ep", "tp", None),
        ),
        out_specs=P("ep", "tp"),
        check_vma=False,
    )
```

```python
import functools

import jax
import jax.numpy as jnp
from jax import lax
from jax.experimental import pallas as pl
from jax.experimental.pallas import tpu as pltpu
from jax.sharding import PartitionSpec as P

MESH = pl.DeviceIdType.MESH
CHUNKS = 4


def each(count, body):
    if count <= 8:
        for i in range(count):
            body(i)
    else:
        pl.loop(0, count)(body)


def partner(t, j, count):
    if count & (count - 1):
        return lax.rem(t + j, count)
    out, bit = 0, 1
    while bit < count:
        have = (t // bit) % 2
        out = out + ((have + 1) % 2 if j & bit else have) * bit
        bit *= 2
    return out


def kernel(
    n_ep, n_tp,
    tok_hbm, cho_hbm, wt_hbm, gate_hbm, up_hbm, down_hbm,
    out_ref,
    tok, cho, wt, gate, up, down,
    leaving, arrived, gate_acc, up_acc, place,
    part_out, part_in, back_out, back_in,
    in_sem, w_sem, d_sem,
    s1_send, s1_recv, s2_send, s2_recv, s3_send, s3_recv,
):
    e = lax.axis_index("ep")
    t = lax.axis_index("tp")
    tok_count, width = tok.shape
    experts, picks = cho.shape
    rows = experts * picks
    cw = width // CHUNKS
    sw = width // n_tp
    hid = gate.shape[1]

    def ep_peer(j):
        low = n_ep - 1 - j
        low = jnp.where(low > e, low, low - 1)
        high = jnp.where(j < e, j, j + 1)
        return jnp.where(e < n_ep // 2, low, high)

    barrier = pltpu.get_barrier_semaphore()

    def greet(j):
        pl.semaphore_signal(barrier, inc=1, device_id={"ep": ep_peer(j)}, device_id_type=MESH)

    each(n_ep - 1, greet)
    for j in range(1, n_tp):
        pl.semaphore_signal(
            barrier, inc=1, device_id={"tp": partner(t, j, n_tp)}, device_id_type=MESH
        )

    loads = [
        pltpu.make_async_copy(cho_hbm.at[e], cho, in_sem.at[0]),
        pltpu.make_async_copy(wt_hbm.at[0], wt, in_sem.at[1]),
        pltpu.make_async_copy(tok_hbm, tok, in_sem.at[2]),
    ]
    for c in loads:
        c.start()
    wloads = []
    for k in range(CHUNKS):
        piece = pl.ds(k * cw, cw)
        a = pltpu.make_async_copy(gate_hbm.at[0, piece, :], gate.at[piece, :], w_sem.at[0, k])
        b = pltpu.make_async_copy(up_hbm.at[0, piece, :], up.at[piece, :], w_sem.at[1, k])
        wloads.append((a, b))
    order = [*range(n_tp - 1, 0, -1), 0]
    dloads = {}
    for j in order:
        col = pl.multiple_of(partner(t, j, n_tp) * sw, sw)
        dloads[j] = pltpu.make_async_copy(
            down_hbm.at[0, :, pl.ds(col, sw)], down.at[j], d_sem.at[j]
        )

    for c in loads:
        c.wait()
    lane = lax.broadcasted_iota(jnp.int32, (picks, picks), 1)
    sub = lax.broadcasted_iota(jnp.int32, (picks, picks), 0)
    diag = lane == sub
    position = lax.broadcasted_iota(jnp.int32, (picks, tok_count), 1).astype(jnp.float32)
    hots, parts = [], []
    for x in range(experts):
        spread = jnp.broadcast_to(cho[x : x + 1, :], (picks, picks)).astype(jnp.float32)
        column = jnp.sum(jnp.where(diag, spread, 0.0), axis=1, keepdims=True)
        wide = jnp.broadcast_to(wt[x : x + 1, :], (picks, picks))
        wcol = jnp.sum(jnp.where(diag, wide, 0.0), axis=1, keepdims=True)
        hit = position == column
        hots.append(jnp.where(hit, 1.0, 0.0))
        parts.append(jnp.where(hit, wcol, 0.0))
    onehot = jnp.concatenate(hots, axis=0).astype(jnp.bfloat16)
    for k in range(CHUNKS):
        sel = jnp.dot(
            onehot, tok[:, k * cw : (k + 1) * cw], preferred_element_type=jnp.float32
        )
        leaving[k] = sel.reshape(experts, picks, cw).astype(jnp.bfloat16)

    pl.semaphore_wait(barrier, n_ep - 1 + n_tp - 1)

    def send_tokens(k, j):
        p = ep_peer(j)
        return pltpu.make_async_remote_copy(
            src_ref=leaving.at[k, p],
            dst_ref=arrived.at[k, e],
            send_sem=s1_send.at[k, j],
            recv_sem=s1_recv.at[k, e],
            device_id={"ep": p},
            device_id_type=MESH,
        )

    for k in range(CHUNKS):
        each(n_ep - 1, lambda j: send_tokens(k, j).start())
    for a, b in wloads:
        a.start()
        b.start()
    for j in order:
        dloads[j].start()

    weighted = jnp.concatenate(parts, axis=0)
    hi = weighted.astype(jnp.bfloat16).astype(jnp.float32)
    mid = (weighted - hi).astype(jnp.bfloat16).astype(jnp.float32)
    lo = weighted - hi - mid
    for i, piece in enumerate((hi, mid, lo)):
        place[i] = piece.T.astype(jnp.bfloat16)

    def rows_in(ref, k, sem, p):
        pltpu.make_async_remote_copy(
            src_ref=ref.at[k, p] if k is not None else ref.at[p],
            dst_ref=ref.at[k, p] if k is not None else ref.at[p],
            send_sem=sem.at[k, p] if k is not None else sem.at[p],
            recv_sem=sem.at[k, p] if k is not None else sem.at[p],
            device_id={"ep": p},
            device_id_type=MESH,
        ).wait_recv()

    for k in range(CHUNKS):
        arrived[k, e] = leaving[k, e]
        each(n_ep - 1, lambda j: rows_in(arrived, k, s1_recv, ep_peer(j)))
        x = arrived[k].astype(jnp.float32).reshape(rows, cw).astype(jnp.bfloat16)
        for c in wloads[k]:
            c.wait()
        g = jnp.dot(x, gate[k * cw : (k + 1) * cw, :], preferred_element_type=jnp.float32)
        u = jnp.dot(x, up[k * cw : (k + 1) * cw, :], preferred_element_type=jnp.float32)
        if k == 0:
            gate_acc[...] = g
            up_acc[...] = u
        else:
            gate_acc[...] += g
            up_acc[...] += u
    g = gate_acc[...]
    hidden = (g / (1.0 + jnp.exp(-g)) * up_acc[...]).astype(jnp.bfloat16)

    sends = []
    for j in order:
        dloads[j].wait()
        part_out[j] = jnp.dot(hidden, down[j], preferred_element_type=jnp.float32).astype(
            jnp.bfloat16
        )
        if j:
            c = pltpu.make_async_remote_copy(
                src_ref=part_out.at[j],
                dst_ref=part_in.at[j - 1],
                send_sem=s2_send.at[j - 1],
                recv_sem=s2_recv.at[j - 1],
                device_id={"tp": partner(t, j, n_tp)},
                device_id_type=MESH,
            )
            c.start()
            sends.append(c)
    total = part_out[0].astype(jnp.float32)
    for c in sends:
        c.wait_recv()
    for j in range(1, n_tp):
        total += part_in[j - 1].astype(jnp.float32)
    back_out[...] = total.reshape(n_ep, picks, sw).astype(jnp.bfloat16)

    def send_back(j):
        p = ep_peer(j)
        return pltpu.make_async_remote_copy(
            src_ref=back_out.at[p],
            dst_ref=back_in.at[e],
            send_sem=s3_send.at[j],
            recv_sem=s3_recv.at[e],
            device_id={"ep": p},
            device_id_type=MESH,
        )

    each(n_ep - 1, lambda j: send_back(j).start())
    back_in[e] = back_out[e]
    each(n_ep - 1, lambda j: rows_in(back_in, None, s3_recv, ep_peer(j)))
    y = back_in[...].astype(jnp.float32).reshape(rows, sw).astype(jnp.bfloat16)
    result = jnp.dot(place[0], y, preferred_element_type=jnp.float32)
    result += jnp.dot(place[1], y, preferred_element_type=jnp.float32)
    result += jnp.dot(place[2], y, preferred_element_type=jnp.float32)
    out_ref[...] = result.astype(out_ref.dtype)

    for k in range(CHUNKS):
        each(n_ep - 1, lambda j: send_tokens(k, j).wait_send())
    for c in sends:
        c.wait_send()
    each(n_ep - 1, lambda j: send_back(j).wait_send())


def local(tokens, chosen, chosen_weight, gate_weight, up_weight, down_weight):
    n_ep, n_tp = lax.axis_size("ep"), lax.axis_size("tp")
    tok_count, width = tokens.shape
    blocks, experts, picks = chosen.shape
    hid = gate_weight.shape[2]
    rows = blocks * picks
    cw, sw = width // CHUNKS, width // n_tp
    bf, f32 = jnp.bfloat16, jnp.float32
    dma = pltpu.SemaphoreType.DMA
    hbm = pl.BlockSpec(memory_space=pltpu.HBM)
    return pl.pallas_call(
        functools.partial(kernel, n_ep, n_tp),
        out_shape=jax.ShapeDtypeStruct((tok_count, sw), bf),
        in_specs=[hbm] * 6,
        out_specs=pl.BlockSpec(memory_space=pltpu.VMEM),
        scratch_shapes=[
            pltpu.VMEM((tok_count, width), bf),
            pltpu.VMEM((experts, picks), jnp.int32),
            pltpu.VMEM((experts, picks), f32),
            pltpu.VMEM((width, hid), bf),
            pltpu.VMEM((width, hid), bf),
            pltpu.VMEM((n_tp, hid, sw), bf),
            pltpu.VMEM((CHUNKS, experts, picks, cw), bf),
            pltpu.VMEM((CHUNKS, blocks, picks, cw), bf),
            pltpu.VMEM((rows, hid), f32),
            pltpu.VMEM((rows, hid), f32),
            pltpu.VMEM((3, tok_count, experts * picks), bf),
            pltpu.VMEM((n_tp, rows, sw), bf),
            pltpu.VMEM((n_tp - 1, rows, sw), bf),
            pltpu.VMEM((blocks, picks, sw), bf),
            pltpu.VMEM((experts, picks, sw), bf),
            dma((3,)),
            dma((2, CHUNKS)),
            dma((n_tp,)),
            dma((CHUNKS, n_ep)),
            dma((CHUNKS, n_ep)),
            dma((n_tp,)),
            dma((n_tp,)),
            dma((n_ep,)),
            dma((n_ep,)),
        ],
        compiler_params=pltpu.CompilerParams(
            collective_id=0, has_side_effects=True, vmem_limit_bytes=32 * 1024 * 1024
        ),
    )(*(
        pltpu.with_memory_space_constraint(a, pltpu.HBM)
        for a in (tokens, chosen, chosen_weight, gate_weight, up_weight, down_weight)
    ))


def solution(mesh):
    return jax.shard_map(
        local,
        mesh=mesh,
        in_specs=(
            P("ep", None),
            P(),
            P("ep", None, None),
            P("ep", None, "tp"),
            P("ep", None, "tp"),
            P("ep", "tp", None),
        ),
        out_specs=P("ep", "tp"),
        check_vma=False,
    )
```

```python
import functools

import jax
import jax.numpy as jnp
from jax import lax
from jax.experimental import pallas as pl
from jax.experimental.pallas import tpu as pltpu
from jax.sharding import PartitionSpec as P

MESH = pl.DeviceIdType.MESH
CHUNKS = 2


def each(count, body):
    if count <= 8:
        for i in range(count):
            body(i)
    else:
        pl.loop(0, count)(body)


def partner(t, j, count):
    if count & (count - 1):
        return lax.rem(t + j, count)
    out, bit = 0, 1
    while bit < count:
        have = (t // bit) % 2
        out = out + ((have + 1) % 2 if j & bit else have) * bit
        bit *= 2
    return out


def kernel(
    n_ep, n_tp,
    tok_hbm, cho_hbm, wt_hbm, gate_hbm, up_hbm, down_hbm,
    out_ref,
    tok, cho, wt, gate, up, down,
    leaving, arrived, gate_acc, up_acc, place,
    part_out, part_in, back_out, back_in,
    in_sem, w_sem, d_sem,
    s1_send, s1_recv, s2_send, s2_recv, s3_send, s3_recv,
):
    e = lax.axis_index("ep")
    t = lax.axis_index("tp")
    tok_count, width = tok.shape
    experts, picks = cho.shape
    rows = experts * picks
    cw = width // CHUNKS
    sw = width // n_tp
    half = n_ep // 2
    far = jnp.where(e < half, 1, 0)

    def ep_peer(j):
        low = n_ep - 1 - j
        low = jnp.where(low > e, low, low - 1)
        high = jnp.where(j < e, j, j + 1)
        return jnp.where(e < half, low, high)

    barrier = pltpu.get_barrier_semaphore()

    def greet(j):
        pl.semaphore_signal(barrier, inc=1, device_id={"ep": ep_peer(j)}, device_id_type=MESH)

    each(n_ep - 1, greet)
    for j in range(1, n_tp):
        pl.semaphore_signal(
            barrier, inc=1, device_id={"tp": partner(t, j, n_tp)}, device_id_type=MESH
        )

    loads = [
        pltpu.make_async_copy(cho_hbm.at[e], cho, in_sem.at[0]),
        pltpu.make_async_copy(wt_hbm.at[0], wt, in_sem.at[1]),
        pltpu.make_async_copy(tok_hbm, tok, in_sem.at[2]),
    ]
    for c in loads:
        c.start()
    wloads = []
    for k in range(CHUNKS):
        piece = pl.ds(k * cw, cw)
        a = pltpu.make_async_copy(gate_hbm.at[0, piece, :], gate.at[piece, :], w_sem.at[0, k])
        b = pltpu.make_async_copy(up_hbm.at[0, piece, :], up.at[piece, :], w_sem.at[1, k])
        wloads.append((a, b))
    order = [*range(n_tp - 1, 0, -1), 0]
    dloads = {}
    for j in order:
        col = pl.multiple_of(partner(t, j, n_tp) * sw, sw)
        dloads[j] = pltpu.make_async_copy(
            down_hbm.at[0, :, pl.ds(col, sw)], down.at[j], d_sem.at[j]
        )

    for c in loads:
        c.wait()
    lane = lax.broadcasted_iota(jnp.int32, (picks, picks), 1)
    sub = lax.broadcasted_iota(jnp.int32, (picks, picks), 0)
    diag = lane == sub
    position = lax.broadcasted_iota(jnp.int32, (picks, tok_count), 1).astype(jnp.float32)
    hots, parts = [], []
    for x in range(experts):
        spread = jnp.broadcast_to(cho[x : x + 1, :], (picks, picks)).astype(jnp.float32)
        column = jnp.sum(jnp.where(diag, spread, 0.0), axis=1, keepdims=True)
        wide = jnp.broadcast_to(wt[x : x + 1, :], (picks, picks))
        wcol = jnp.sum(jnp.where(diag, wide, 0.0), axis=1, keepdims=True)
        hit = position == column
        hots.append(jnp.where(hit, 1.0, 0.0))
        parts.append(jnp.where(hit, wcol, 0.0))
    onehot = jnp.concatenate(hots, axis=0).astype(jnp.bfloat16)
    for k in range(CHUNKS):
        sel = jnp.dot(
            onehot, tok[:, k * cw : (k + 1) * cw], preferred_element_type=jnp.float32
        )
        leaving[k] = sel.reshape(experts, picks, cw).astype(jnp.bfloat16)

    pl.semaphore_wait(barrier, n_ep - 1 + n_tp - 1)

    def send_tokens(k, j):
        p = ep_peer(j)
        return pltpu.make_async_remote_copy(
            src_ref=leaving.at[k, p],
            dst_ref=arrived.at[k, e],
            send_sem=s1_send.at[k, j],
            recv_sem=s1_recv.at[k, e],
            device_id={"ep": p},
            device_id_type=MESH,
        )

    for k in range(CHUNKS):
        each(n_ep - 1, lambda j: send_tokens(k, j).start())
    for a, b in wloads:
        a.start()
        b.start()
    for j in order:
        dloads[j].start()

    weighted = jnp.concatenate(parts, axis=0)
    hi = weighted.astype(jnp.bfloat16).astype(jnp.float32)
    mid = (weighted - hi).astype(jnp.bfloat16).astype(jnp.float32)
    lo = weighted - hi - mid
    for i, piece in enumerate((hi, mid, lo)):
        place[i] = piece.T.astype(jnp.bfloat16)

    def rows_in(ref, k, sem, p):
        pltpu.make_async_remote_copy(
            src_ref=ref.at[k, p] if k is not None else ref.at[p],
            dst_ref=ref.at[k, p] if k is not None else ref.at[p],
            send_sem=sem.at[k, p] if k is not None else sem.at[p],
            recv_sem=sem.at[k, p] if k is not None else sem.at[p],
            device_id={"ep": p},
            device_id_type=MESH,
        ).wait_recv()

    for k in range(CHUNKS):
        arrived[k, e] = leaving[k, e]
        each(n_ep - 1, lambda j: rows_in(arrived, k, s1_recv, ep_peer(j)))
        x = arrived[k].astype(jnp.float32).reshape(rows, cw).astype(jnp.bfloat16)
        for c in wloads[k]:
            c.wait()
        g = jnp.dot(x, gate[k * cw : (k + 1) * cw, :], preferred_element_type=jnp.float32)
        u = jnp.dot(x, up[k * cw : (k + 1) * cw, :], preferred_element_type=jnp.float32)
        if k == 0:
            gate_acc[...] = g
            up_acc[...] = u
        else:
            gate_acc[...] += g
            up_acc[...] += u
    g = gate_acc[...]
    hidden = (g / (1.0 + jnp.exp(-g)) * up_acc[...]).astype(jnp.bfloat16)

    def send_part(h, j):
        side = far if h == 0 else 1 - far
        return pltpu.make_async_remote_copy(
            src_ref=part_out.at[j, side],
            dst_ref=part_in.at[j - 1, side],
            send_sem=s2_send.at[h, j],
            recv_sem=s2_recv.at[h, j],
            device_id={"tp": partner(t, j, n_tp)},
            device_id_type=MESH,
        )

    def send_back(j):
        p = ep_peer(j)
        return pltpu.make_async_remote_copy(
            src_ref=back_out.at[p],
            dst_ref=back_in.at[e],
            send_sem=s3_send.at[j],
            recv_sem=s3_recv.at[e],
            device_id={"ep": p},
            device_id_type=MESH,
        )

    for j in order:
        dloads[j].wait()
        part = jnp.dot(hidden, down[j], preferred_element_type=jnp.float32)
        part_out[j] = part.reshape(2, rows // 2, sw).astype(jnp.bfloat16)
        if j:
            send_part(0, j).start()
        if j == 1:
            for i in range(n_tp - 1, 0, -1):
                send_part(1, i).start()
    for h in range(2):
        side = far if h == 0 else 1 - far
        total = part_out[0, side].astype(jnp.float32)
        for j in range(n_tp - 1, 0, -1):
            send_part(h, j).wait_recv()
            total += part_in[j - 1, side].astype(jnp.float32)
        back_out[pl.ds(side * half, half)] = total.reshape(half, picks, sw).astype(jnp.bfloat16)
        if h == 0:
            each(half, lambda j: send_back(j).start())
        else:
            each(half - 1, lambda j: send_back(j + half).start())
    back_in[e] = back_out[e]
    each(n_ep - 1, lambda j: rows_in(back_in, None, s3_recv, ep_peer(j)))
    y = back_in[...].astype(jnp.float32).reshape(rows, sw).astype(jnp.bfloat16)
    result = jnp.dot(place[0], y, preferred_element_type=jnp.float32)
    result += jnp.dot(place[1], y, preferred_element_type=jnp.float32)
    result += jnp.dot(place[2], y, preferred_element_type=jnp.float32)
    out_ref[...] = result.astype(out_ref.dtype)

    for k in range(CHUNKS):
        each(n_ep - 1, lambda j: send_tokens(k, j).wait_send())
    for j in range(1, n_tp):
        send_part(0, j).wait_send()
        send_part(1, j).wait_send()
    each(n_ep - 1, lambda j: send_back(j).wait_send())


def local(tokens, chosen, chosen_weight, gate_weight, up_weight, down_weight):
    n_ep, n_tp = lax.axis_size("ep"), lax.axis_size("tp")
    tok_count, width = tokens.shape
    blocks, experts, picks = chosen.shape
    hid = gate_weight.shape[2]
    rows = blocks * picks
    cw, sw = width // CHUNKS, width // n_tp
    bf, f32 = jnp.bfloat16, jnp.float32
    dma = pltpu.SemaphoreType.DMA
    hbm = pl.BlockSpec(memory_space=pltpu.HBM)
    return pl.pallas_call(
        functools.partial(kernel, n_ep, n_tp),
        out_shape=jax.ShapeDtypeStruct((tok_count, sw), bf),
        in_specs=[hbm] * 6,
        out_specs=pl.BlockSpec(memory_space=pltpu.VMEM),
        scratch_shapes=[
            pltpu.VMEM((tok_count, width), bf),
            pltpu.VMEM((experts, picks), jnp.int32),
            pltpu.VMEM((experts, picks), f32),
            pltpu.VMEM((width, hid), bf),
            pltpu.VMEM((width, hid), bf),
            pltpu.VMEM((n_tp, hid, sw), bf),
            pltpu.VMEM((CHUNKS, experts, picks, cw), bf),
            pltpu.VMEM((CHUNKS, blocks, picks, cw), bf),
            pltpu.VMEM((rows, hid), f32),
            pltpu.VMEM((rows, hid), f32),
            pltpu.VMEM((3, tok_count, experts * picks), bf),
            pltpu.VMEM((n_tp, 2, rows // 2, sw), bf),
            pltpu.VMEM((n_tp - 1, 2, rows // 2, sw), bf),
            pltpu.VMEM((blocks, picks, sw), bf),
            pltpu.VMEM((experts, picks, sw), bf),
            dma((3,)),
            dma((2, CHUNKS)),
            dma((n_tp,)),
            dma((CHUNKS, n_ep)),
            dma((CHUNKS, n_ep)),
            dma((2, n_tp)),
            dma((2, n_tp)),
            dma((n_ep,)),
            dma((n_ep,)),
        ],
        compiler_params=pltpu.CompilerParams(
            collective_id=0, has_side_effects=True, vmem_limit_bytes=32 * 1024 * 1024
        ),
    )(*(
        pltpu.with_memory_space_constraint(a, pltpu.HBM)
        for a in (tokens, chosen, chosen_weight, gate_weight, up_weight, down_weight)
    ))


def solution(mesh):
    return jax.shard_map(
        local,
        mesh=mesh,
        in_specs=(
            P("ep", None),
            P(),
            P("ep", None, None),
            P("ep", None, "tp"),
            P("ep", None, "tp"),
            P("ep", "tp", None),
        ),
        out_specs=P("ep", "tp"),
        check_vma=False,
    )
```

```python
import functools

import jax
import jax.numpy as jnp
from jax import lax
from jax.experimental import pallas as pl
from jax.experimental.pallas import tpu as pltpu
from jax.sharding import PartitionSpec as P

MESH = pl.DeviceIdType.MESH
CHUNKS = 2


def each(count, body):
    if count <= 8:
        for i in range(count):
            body(i)
    else:
        pl.loop(0, count)(body)


def partner(t, j, count):
    if count & (count - 1):
        return lax.rem(t + j, count)
    out, bit = 0, 1
    while bit < count:
        have = (t // bit) % 2
        out = out + ((have + 1) % 2 if j & bit else have) * bit
        bit *= 2
    return out


def kernel(
    n_ep, n_tp,
    tok_hbm, cho_hbm, wt_hbm, gate_hbm, up_hbm, down_hbm,
    out_ref,
    tok, cho, wt, gate, up, down,
    leaving, arrived, gate_acc, up_acc, place,
    part_out, part_in, back_out, back_in,
    in_sem, w_sem, d_sem,
    s1_send, s1_recv, s2_send, s2_recv, s3_send, s3_recv,
):
    e = lax.axis_index("ep")
    t = lax.axis_index("tp")
    tok_count, width = tok.shape
    experts, picks = cho.shape
    rows = experts * picks
    cw = width // CHUNKS
    sw = width // n_tp
    half = n_ep // 2
    far = jnp.where(e < half, 1, 0)

    def ep_peer(j):
        low = n_ep - 1 - j
        low = jnp.where(low > e, low, low - 1)
        high = jnp.where(j < e, j, j + 1)
        return jnp.where(e < half, low, high)

    barrier = pltpu.get_barrier_semaphore()

    def greet(j):
        pl.semaphore_signal(barrier, inc=1, device_id={"ep": ep_peer(j)}, device_id_type=MESH)

    each(n_ep - 1, greet)
    for j in range(1, n_tp):
        pl.semaphore_signal(
            barrier, inc=1, device_id={"tp": partner(t, j, n_tp)}, device_id_type=MESH
        )

    loads = [
        pltpu.make_async_copy(cho_hbm.at[e], cho, in_sem.at[0]),
        pltpu.make_async_copy(wt_hbm.at[0], wt, in_sem.at[1]),
        pltpu.make_async_copy(tok_hbm, tok, in_sem.at[2]),
    ]
    for c in loads:
        c.start()
    wloads = []
    for k in range(CHUNKS):
        piece = pl.ds(k * cw, cw)
        a = pltpu.make_async_copy(gate_hbm.at[0, piece, :], gate.at[piece, :], w_sem.at[0, k])
        b = pltpu.make_async_copy(up_hbm.at[0, piece, :], up.at[piece, :], w_sem.at[1, k])
        wloads.append((a, b))
    order = [*range(n_tp - 1, 0, -1), 0]
    dloads = {}
    for j in order:
        col = pl.multiple_of(partner(t, j, n_tp) * sw, sw)
        dloads[j] = pltpu.make_async_copy(
            down_hbm.at[0, :, pl.ds(col, sw)], down.at[j], d_sem.at[j]
        )

    for c in loads:
        c.wait()
    lane = lax.broadcasted_iota(jnp.int32, (picks, picks), 1)
    sub = lax.broadcasted_iota(jnp.int32, (picks, picks), 0)
    diag = lane == sub
    position = lax.broadcasted_iota(jnp.int32, (picks, tok_count), 1).astype(jnp.float32)
    hots, parts = [], []
    for x in range(experts):
        spread = jnp.broadcast_to(cho[x : x + 1, :], (picks, picks)).astype(jnp.float32)
        column = jnp.sum(jnp.where(diag, spread, 0.0), axis=1, keepdims=True)
        wide = jnp.broadcast_to(wt[x : x + 1, :], (picks, picks))
        wcol = jnp.sum(jnp.where(diag, wide, 0.0), axis=1, keepdims=True)
        hit = position == column
        hots.append(jnp.where(hit, 1.0, 0.0))
        parts.append(jnp.where(hit, wcol, 0.0))
    onehot = jnp.concatenate(hots, axis=0).astype(jnp.bfloat16)
    for k in range(CHUNKS):
        sel = jnp.dot(
            onehot, tok[:, k * cw : (k + 1) * cw], preferred_element_type=jnp.float32
        )
        leaving[k] = sel.reshape(experts, picks, cw).astype(jnp.bfloat16)

    pl.semaphore_wait(barrier, n_ep - 1 + n_tp - 1)

    def send_tokens(k, j):
        p = ep_peer(j)
        return pltpu.make_async_remote_copy(
            src_ref=leaving.at[k, p],
            dst_ref=arrived.at[k, e],
            send_sem=s1_send.at[k, j],
            recv_sem=s1_recv.at[k, e],
            device_id={"ep": p},
            device_id_type=MESH,
        )

    for k in range(CHUNKS):
        each(n_ep - 1, lambda j: send_tokens(k, j).start())
    for a, b in wloads:
        a.start()
        b.start()
    for j in order:
        dloads[j].start()

    weighted = jnp.concatenate(parts, axis=0)
    hi = weighted.astype(jnp.bfloat16).astype(jnp.float32)
    mid = (weighted - hi).astype(jnp.bfloat16).astype(jnp.float32)
    lo = weighted - hi - mid
    for i, piece in enumerate((hi, mid, lo)):
        place[i] = piece.T.astype(jnp.bfloat16)

    def rows_in(ref, k, sem, p):
        pltpu.make_async_remote_copy(
            src_ref=ref.at[k, p] if k is not None else ref.at[p],
            dst_ref=ref.at[k, p] if k is not None else ref.at[p],
            send_sem=sem.at[k, p] if k is not None else sem.at[p],
            recv_sem=sem.at[k, p] if k is not None else sem.at[p],
            device_id={"ep": p},
            device_id_type=MESH,
        ).wait_recv()

    for k in range(CHUNKS):
        arrived[k, e] = leaving[k, e]
        each(n_ep - 1, lambda j: rows_in(arrived, k, s1_recv, ep_peer(j)))
        x = arrived[k].astype(jnp.float32).reshape(rows, cw).astype(jnp.bfloat16)
        for c in wloads[k]:
            c.wait()
        g = jnp.dot(x, gate[k * cw : (k + 1) * cw, :], preferred_element_type=jnp.float32)
        u = jnp.dot(x, up[k * cw : (k + 1) * cw, :], preferred_element_type=jnp.float32)
        if k == 0:
            gate_acc[...] = g
            up_acc[...] = u
        else:
            gate_acc[...] += g
            up_acc[...] += u
    g = gate_acc[...]
    hidden = (g / (1.0 + jnp.exp(-g)) * up_acc[...]).astype(jnp.bfloat16)

    def send_part(h, j):
        side = far if h == 0 else 1 - far
        return pltpu.make_async_remote_copy(
            src_ref=part_out.at[j, side],
            dst_ref=part_in.at[j - 1, side],
            send_sem=s2_send.at[h, j],
            recv_sem=s2_recv.at[h, j],
            device_id={"tp": partner(t, j, n_tp)},
            device_id_type=MESH,
        )

    def send_back(j):
        p = ep_peer(j)
        return pltpu.make_async_remote_copy(
            src_ref=back_out.at[p],
            dst_ref=back_in.at[e],
            send_sem=s3_send.at[j],
            recv_sem=s3_recv.at[e],
            device_id={"ep": p},
            device_id_type=MESH,
        )

    for j in order:
        dloads[j].wait()
        part = jnp.dot(hidden, down[j], preferred_element_type=jnp.float32)
        part_out[j] = part.reshape(2, rows // 2, sw).astype(jnp.bfloat16)
        if j:
            send_part(0, j).start()
            send_part(1, j).start()
    for h in range(2):
        side = far if h == 0 else 1 - far
        total = part_out[0, side].astype(jnp.float32)
        for j in range(n_tp - 1, 0, -1):
            send_part(h, j).wait_recv()
            total += part_in[j - 1, side].astype(jnp.float32)
        back_out[pl.ds(side * half, half)] = total.reshape(half, picks, sw).astype(jnp.bfloat16)
        if h == 0:
            each(half, lambda j: send_back(j).start())
        else:
            each(half - 1, lambda j: send_back(j + half).start())
    back_in[e] = back_out[e]
    each(n_ep - 1, lambda j: rows_in(back_in, None, s3_recv, ep_peer(j)))
    y = back_in[...].astype(jnp.float32).reshape(rows, sw).astype(jnp.bfloat16)
    terms = jnp.concatenate([place[0], place[1], place[2]], axis=0)
    terms = jnp.dot(terms, y, preferred_element_type=jnp.float32)
    result = terms[:tok_count] + terms[tok_count : 2 * tok_count] + terms[2 * tok_count :]
    out_ref[...] = result.astype(out_ref.dtype)

    for k in range(CHUNKS):
        each(n_ep - 1, lambda j: send_tokens(k, j).wait_send())
    for j in range(1, n_tp):
        send_part(0, j).wait_send()
        send_part(1, j).wait_send()
    each(n_ep - 1, lambda j: send_back(j).wait_send())


def local(tokens, chosen, chosen_weight, gate_weight, up_weight, down_weight):
    n_ep, n_tp = lax.axis_size("ep"), lax.axis_size("tp")
    tok_count, width = tokens.shape
    blocks, experts, picks = chosen.shape
    hid = gate_weight.shape[2]
    rows = blocks * picks
    cw, sw = width // CHUNKS, width // n_tp
    bf, f32 = jnp.bfloat16, jnp.float32
    dma = pltpu.SemaphoreType.DMA
    hbm = pl.BlockSpec(memory_space=pltpu.HBM)
    return pl.pallas_call(
        functools.partial(kernel, n_ep, n_tp),
        out_shape=jax.ShapeDtypeStruct((tok_count, sw), bf),
        in_specs=[hbm] * 6,
        out_specs=pl.BlockSpec(memory_space=pltpu.VMEM),
        scratch_shapes=[
            pltpu.VMEM((tok_count, width), bf),
            pltpu.VMEM((experts, picks), jnp.int32),
            pltpu.VMEM((experts, picks), f32),
            pltpu.VMEM((width, hid), bf),
            pltpu.VMEM((width, hid), bf),
            pltpu.VMEM((n_tp, hid, sw), bf),
            pltpu.VMEM((CHUNKS, experts, picks, cw), bf),
            pltpu.VMEM((CHUNKS, blocks, picks, cw), bf),
            pltpu.VMEM((rows, hid), f32),
            pltpu.VMEM((rows, hid), f32),
            pltpu.VMEM((3, tok_count, experts * picks), bf),
            pltpu.VMEM((n_tp, 2, rows // 2, sw), bf),
            pltpu.VMEM((n_tp - 1, 2, rows // 2, sw), bf),
            pltpu.VMEM((blocks, picks, sw), bf),
            pltpu.VMEM((experts, picks, sw), bf),
            dma((3,)),
            dma((2, CHUNKS)),
            dma((n_tp,)),
            dma((CHUNKS, n_ep)),
            dma((CHUNKS, n_ep)),
            dma((2, n_tp)),
            dma((2, n_tp)),
            dma((n_ep,)),
            dma((n_ep,)),
        ],
        compiler_params=pltpu.CompilerParams(
            collective_id=0, has_side_effects=True, vmem_limit_bytes=32 * 1024 * 1024
        ),
    )(*(
        pltpu.with_memory_space_constraint(a, pltpu.HBM)
        for a in (tokens, chosen, chosen_weight, gate_weight, up_weight, down_weight)
    ))


def solution(mesh):
    return jax.shard_map(
        local,
        mesh=mesh,
        in_specs=(
            P("ep", None),
            P(),
            P("ep", None, None),
            P("ep", None, "tp"),
            P("ep", None, "tp"),
            P("ep", "tp", None),
        ),
        out_specs=P("ep", "tp"),
        check_vma=False,
    )
```
